32 devices in a mesh: grp: 2 (over y), fs: 4 (over z), tp: 4 (over x, core).
Axes of the slice: x: 2, y: 2, z: 4, core: 2. Of those that a mesh axis runs over, the one named last changes fastest.
Arguments:
- tokens: bfloat16 [2048, 2048], P(('grp', 'fs', 'tp')), parts along dimension 0, may hold values from -30 to 30
- gate_master: float32 [2048, 2752], P('fs', 'tp'), may hold values from -0.125 to 0.125
- up_master: float32 [2048, 2752], P('fs', 'tp'), may hold values from -0.125 to 0.125
- down_master: float32 [2048, 2752], P('fs', 'tp'), may hold values from -0.4375 to 0.4375
- norm_gain: float32 [2048], replicated, may hold values from 0.1 to 1.9
- post_gain: float32 [2048], replicated, may hold values from 0.1 to 1.9
- post_bias: float32 [2048], replicated, may hold values from -3 to 3
Outputs:
- gate_ready: bfloat16 [4096, 2752], P('grp', 'tp'), parts along dimension 0
- up_ready: bfloat16 [4096, 2752], P('grp', 'tp'), parts along dimension 0
- down_ready: bfloat16 [4096, 2752], P('grp', 'tp'), parts along dimension 0
- result: bfloat16 [2048, 2048], P(('grp', 'fs', 'tp')), parts along dimension 0
The draws below stay inside these ranges and needn't reach their ends.
There are 2 independent parts, one for each index of `grp`. The reference program is written for one: setup_inputs(seed, part) draws one part's arguments, and reference() takes and returns one part's arrays. A program takes and returns all parts, laid end to end along the dimension named above; an argument that names none is the same for every part. Nothing has to cross between parts.
All inputs are finite; a program needn't handle non-finite values.
Results may differ from the reference program's by a relative error of at most 0.009.
Values may be sent and summed in bfloat16 or wider, within the bound.
No kernel may reach another device: no remote copies, remote signals or barrier semaphores. Data moves between devices by JAX's collectives and lax.ppermute only.
A program may use at most 64 MiB of HBM per device.

```python
import math
import jax
import jax.numpy as jnp
from jax import lax

D = 2048
FF = 2752
TOKENS = 1024
N_TP = 4


def draw_tokens(key, part):
    key_base, key_rows, key_cols = jax.random.split(key, 3)
    row_scale = jnp.exp(jax.random.uniform(key_rows, (TOKENS, 1), jnp.float32, math.log(0.3), math.log(3.0)))
    col_scale = jnp.exp(jax.random.uniform(key_cols, (1, D), jnp.float32, math.log(0.5), math.log(2.0)))
    base = jnp.clip(jax.random.normal(key_base, (TOKENS, D), jnp.float32), -4.0, 4.0)
    return (base * row_scale * col_scale).astype(jnp.bfloat16)


def shard_levels(rng, dims, pieces, least, top_value):
    gain = 1.0
    for axis_at, parts in pieces:
        draws = jax.random.uniform(jax.random.fold_in(jax.random.fold_in(rng, 6), axis_at), (parts,), jnp.float32, least / len(pieces), top_value / len(pieces))
        gain = gain * jnp.repeat(jnp.exp(draws), dims[axis_at] // parts).reshape((-1,) + (1,) * (len(dims) - 1 - axis_at))
    return gain


def centred(key, shape, deviation, most, cuts=(), kind=jnp.bfloat16):
    values = deviation * jax.random.normal(key, shape, jnp.float32)
    if cuts:
        values = values * shard_levels(key, shape, cuts, -0.22, 0.18)
    return jnp.clip(values, -most, most).astype(kind)


def setup_inputs(seed: int = 0, part: int = 0) -> dict:
    streams_of = jax.random.split(jax.random.key(seed), 8)
    part_keys = jax.random.split(jax.random.fold_in(streams_of[7], part), 8)
    return {
        "tokens": draw_tokens(jax.random.fold_in(jax.random.fold_in(streams_of[7], part), 71), part),
        "gate_master": centred(streams_of[1], (D, FF), D ** -0.5, 0.125, ((0, 4), (1, 4)), jnp.float32),
        "up_master": centred(streams_of[2], (D, FF), D ** -0.5, 0.125, ((0, 4), (1, 4)), jnp.float32),
        "down_master": centred(streams_of[3], (D, FF), (FF // 16) ** -0.5, 0.4375, ((0, 4), (1, 4)), jnp.float32),
        "norm_gain": jnp.clip(1.0 + 0.18 * jax.random.normal(streams_of[4], (D,), jnp.float32), 0.1, 1.9),
        "post_gain": jnp.clip(1.0 + 0.18 * jax.random.normal(streams_of[5], (D,), jnp.float32), 0.1, 1.9),
        "post_bias": centred(streams_of[6], (D,), 0.5, 3.0, (), jnp.float32),
    }


def reference(tokens, gate_master, up_master, down_master, norm_gain, post_gain, post_bias):
    gate_ready = (norm_gain[:, None] * gate_master).astype(jnp.bfloat16)
    up_ready = (norm_gain[:, None] * up_master).astype(jnp.bfloat16)
    down_ready = down_master.astype(jnp.bfloat16)
    wide = tokens.astype(jnp.float32)
    normed = (wide * lax.rsqrt(lax.optimization_barrier(jnp.mean(wide * wide, axis=-1, keepdims=True)) + 1e-06)).astype(jnp.bfloat16)
    gate = jnp.dot(normed, gate_ready, preferred_element_type=jnp.float32)
    upward = jnp.dot(normed, up_ready, preferred_element_type=jnp.float32)
    hidden = (jax.nn.silu(gate) * upward).astype(jnp.bfloat16)
    block_units = FF // N_TP
    branch = jnp.zeros((tokens.shape[0], D), jnp.float32)
    for block in range(N_TP):
        part_hidden = hidden[:, block * block_units:(block + 1) * block_units]
        part_down = down_ready[:, block * block_units:(block + 1) * block_units]
        partial_value = lax.dot_general(part_hidden, part_down, (((1,), (1,)), ((), ())), preferred_element_type=jnp.float32)
        rounded = lax.optimization_barrier(partial_value.astype(jnp.bfloat16))
        branch = branch + rounded.astype(jnp.float32)
    mixed = jnp.sqrt(jnp.float32(2.0)) * wide + 0.5 * branch
    center = lax.optimization_barrier(jnp.mean(mixed, axis=-1, keepdims=True))
    spread = lax.optimization_barrier(jnp.mean(jnp.square(mixed - center), axis=-1, keepdims=True))
    result = ((mixed - center) * lax.rsqrt(spread + 1e-05) * post_gain + post_bias).astype(jnp.bfloat16)
    return (gate_ready, up_ready, down_ready, result)
```

```python
import functools

import jax
import jax.numpy as jnp
from jax import lax
from jax.experimental import pallas as pl
from jax.experimental.pallas import tpu as pltpu
from jax.sharding import PartitionSpec as P


BF16 = jnp.bfloat16
F32 = jnp.float32
ANY = pl.BlockSpec(memory_space=pl.ANY)
VMEM = pl.BlockSpec(memory_space=pltpu.VMEM)
LANES = 128
LONGEST_LINE = 8


def finish(wide, branch, post_gain, post_bias):
    mixed = jnp.sqrt(jnp.float32(2.0)) * wide + 0.5 * branch
    center = jnp.mean(mixed, axis=-1, keepdims=True)
    spread = jnp.mean(jnp.square(mixed - center), axis=-1, keepdims=True)
    return ((mixed - center) * lax.rsqrt(spread + 1e-05) * post_gain + post_bias).astype(
        jnp.bfloat16
    )


def plain(tokens, gate_master, up_master, down_master, norm_gain, post_gain, post_bias):
    row_count = gate_master.shape[0]
    first_row = lax.axis_index("fs") * row_count
    gain_rows = lax.dynamic_slice_in_dim(norm_gain, first_row, row_count, 0)
    gate_piece = (gain_rows[:, None] * gate_master).astype(BF16)
    up_piece = (gain_rows[:, None] * up_master).astype(BF16)
    down_piece = down_master.astype(BF16)
    gate_ready, up_ready, down_ready = (
        lax.all_gather(gate_piece, "fs", axis=0, tiled=True),
        lax.all_gather(up_piece, "fs", axis=0, tiled=True),
        lax.all_gather(down_piece, "fs", axis=0, tiled=True),
    )
    wide = tokens.astype(F32)
    normed = (wide * lax.rsqrt(jnp.mean(wide * wide, axis=-1, keepdims=True) + 1e-06)).astype(BF16)
    piece = lax.all_gather(normed, "tp", axis=0, tiled=True)
    gate = jnp.dot(piece, gate_ready, preferred_element_type=F32)
    upward = jnp.dot(piece, up_ready, preferred_element_type=F32)
    hidden = (jax.nn.silu(gate) * upward).astype(BF16)
    branch = lax.psum_scatter(
        lax.dot_general(
            hidden, down_ready, (((1,), (1,)), ((), ())), preferred_element_type=F32
        ).astype(BF16),
        "tp",
        scatter_dimension=0,
        tiled=True,
    ).astype(F32)
    return (gate_ready, up_ready, down_ready, finish(wide, branch, post_gain, post_bias))


class Line:
    def __init__(self, count):
        self.count = count
        self.swaps = []
        self.pairs = {}
        self.brings = {}
        for t in range(1, count):
            for q in (0, 1):
                pairs, brings = [], {}
                for i in range(q, count - 1, 2):
                    if i - t + 1 >= 0:
                        pairs.append((i, i + 1))
                        brings[i + 1] = i + 1 - t
                    if i + t < count:
                        pairs.append((i + 1, i))
                        brings[i] = i + t
                if pairs:
                    self.swaps.append((t, q))
                    self.pairs[t, q] = pairs
                    self.brings[t, q] = brings
        self.order = {f: [s for s in self.swaps if f in self.brings[s]] for f in range(count)}
        self.slots = [
            sorted({self.order[f][k] for f in range(count)}) for k in range(count - 1)
        ]

    def piece(self, f, k):
        out = jnp.int32(0)
        for i in range(self.count):
            s = self.order[i][k]
            out = jnp.where(f == i, jnp.int32(self.brings[s][i]), out)
        return out

    def holds(self, f, k, s):
        out = f < 0
        for i in range(self.count):
            if self.order[i][k] == s:
                out = jnp.logical_or(out, f == i)
        return out


def line_exchange(line, half, groups):
    near, far = {}, {}
    for t, q in line.swaps:
        operand = half if t == 1 else near[t - 1, 1 - q]
        near[t, q] = lax.ppermute(operand, "fs", line.pairs[t, q])
        across = [
            (g * line.count + f, ((g + 1) % groups) * line.count + f)
            for g in range(groups)
            for f in line.brings[t, q]
        ]
        far[t, q] = lax.ppermute(near[t, q], ("grp", "fs"), across)
    return near, far


def at(start, size):
    return pl.ds(pl.multiple_of(start, LANES), size)


def cost(flops, moved):
    return pl.CostEstimate(flops=flops, bytes_accessed=moved, transcendentals=0)


def half_pair_kernel(gate_ref, up_ref, gain_ref, out_ref, buf, sem):
    half = out_ref.shape[-1]
    whole = gate_ref.shape[-1]
    g, f = lax.axis_index("grp"), lax.axis_index("fs")
    loads = [
        pltpu.make_async_copy(src.at[:, at(g * half, half)], buf.at[n], sem.at[n])
        for n, src in enumerate((gate_ref, up_ref))
    ]
    for load in loads:
        load.start()
    gain = gain_ref[:, at(f * whole + g * half, half)]
    for n, load in enumerate(loads):
        load.wait()
        out_ref[n] = (buf[n] * gain).astype(BF16)


def half_pair(gate, up, gain, groups):
    units, whole = gate.shape
    half = whole // groups
    return pl.pallas_call(
        half_pair_kernel,
        out_shape=jax.ShapeDtypeStruct((2, units, half), BF16),
        in_specs=[ANY, ANY, VMEM],
        out_specs=VMEM,
        scratch_shapes=[pltpu.VMEM((2, units, half), F32), pltpu.SemaphoreType.DMA((2,))],
        cost_estimate=cost(2 * units * half, 12 * units * half),
        name="half_pair",
    )(gate, up, gain)


def half_down_kernel(down_ref, out_ref, buf, sem):
    half = out_ref.shape[-1]
    g = lax.axis_index("grp")
    load = pltpu.make_async_copy(down_ref.at[:, at(g * half, half)], buf, sem)
    load.start()
    load.wait()
    out_ref[...] = buf[...].astype(BF16)


def half_down(down, groups):
    units, whole = down.shape
    half = whole // groups
    return pl.pallas_call(
        half_down_kernel,
        out_shape=jax.ShapeDtypeStruct((units, half), BF16),
        in_specs=[ANY],
        out_specs=VMEM,
        scratch_shapes=[pltpu.VMEM((units, half), F32), pltpu.SemaphoreType.DMA],
        cost_estimate=cost(units * half, 6 * units * half),
        name="half_down",
    )(down)


def norm_kernel(tokens_ref, out_ref):
    wide = tokens_ref[...].astype(F32)
    scale = lax.rsqrt(jnp.mean(wide * wide, axis=-1, keepdims=True) + 1e-06)
    out_ref[...] = (wide * scale).astype(BF16)


def norm(tokens):
    return pl.pallas_call(
        norm_kernel,
        out_shape=jax.ShapeDtypeStruct(tokens.shape, BF16),
        in_specs=[VMEM],
        out_specs=VMEM,
        cost_estimate=cost(4 * tokens.size, 4 * tokens.size),
        name="norm_tokens",
    )(tokens)


def slot_loads(line, f, k, refs, fill, sem):
    swaps = line.slots[k]

    def each(act):
        for s in swaps:
            if len(swaps) == 1:
                act(pltpu.make_async_copy(refs[s], fill, sem))
            else:

                @pl.when(line.holds(f, k, s))
                def _():
                    act(pltpu.make_async_copy(refs[s], fill, sem))

    return (lambda: each(lambda c: c.start())), (lambda: each(lambda c: c.wait()))


def pair_kernel(line, n_tok, *refs):
    swaps = line.swaps
    toks, refs = refs[:n_tok], refs[n_tok:]
    (gate_ref, up_ref, gain_ref), refs = refs[:3], refs[3:]
    near, refs = dict(zip(swaps, refs)), refs[len(swaps):]
    far, refs = dict(zip(swaps, refs)), refs[len(swaps):]
    gate_out, up_out, hidden_ref, normed, held, masters, sem_in, sem_m, sem_t, sem_out = refs
    g, f = lax.axis_index("grp"), lax.axis_index("fs")
    whole = gate_ref.shape[-1]
    half = near[swaps[0]].shape[-1]
    rows = toks[0].shape[0]
    mine = [
        pltpu.make_async_copy(src, masters.at[n], sem_m.at[n])
        for n, src in enumerate((gate_ref, up_ref))
    ]
    for load in mine:
        load.start()
    loads = []
    for k in range(line.count - 1):
        start = line.piece(f, k) * whole
        for side, (table, h) in enumerate(((near, g), (far, 1 - g))):
            loads.append(
                slot_loads(
                    line, f, k, table, held.at[:, :, at(start + h * half, half)],
                    sem_in.at[2 * k + side],
                )
            )
    for begin, _ in loads:
        begin()
    token_loads = [
        pltpu.make_async_copy(tok, normed.at[pl.ds(d * rows, rows)], sem_t.at[d])
        for d, tok in enumerate(toks)
    ]
    for load in token_loads:
        load.start()
    gain = gain_ref[:, at(f * whole, whole)]
    for n, load in enumerate(mine):
        load.wait()
        held[n, :, at(f * whole, whole)] = (masters[n] * gain).astype(BF16)
    for _, end in loads:
        end()
    stores = [
        pltpu.make_async_copy(held.at[n], out, sem_out.at[n])
        for n, out in enumerate((gate_out, up_out))
    ]
    for store in stores:
        store.start()
    for load in token_loads:
        load.wait()
    both = [
        lax.dot_general(
            normed[...], held[n], (((1,), (1,)), ((), ())), preferred_element_type=F32
        )
        for n in range(2)
    ]
    gate, up = both
    hidden_ref[...] = (gate / (1.0 + jnp.exp(-gate)) * up).astype(BF16)
    for store in stores:
        store.wait()


def pair(line, toks, gate, up, gain, near, far):
    units, whole = gate.shape
    width = whole * line.count
    n_tok = len(toks)
    rows = toks[0].shape[0]
    slots = line.count - 1
    return pl.pallas_call(
        functools.partial(pair_kernel, line, n_tok),
        out_shape=(
            jax.ShapeDtypeStruct((units, width), BF16),
            jax.ShapeDtypeStruct((units, width), BF16),
            jax.ShapeDtypeStruct((n_tok * rows, units), BF16),
        ),
        in_specs=[ANY] * (n_tok + 2) + [VMEM] + [ANY] * (2 * len(line.swaps)),
        out_specs=(ANY, ANY, VMEM),
        scratch_shapes=[
            pltpu.VMEM((n_tok * rows, width), BF16),
            pltpu.VMEM((2, units, width), BF16),
            pltpu.VMEM((2, units, whole), F32),
            pltpu.SemaphoreType.DMA((2 * slots,)),
            pltpu.SemaphoreType.DMA((2,)),
            pltpu.SemaphoreType.DMA((n_tok,)),
            pltpu.SemaphoreType.DMA((2,)),
        ],
        cost_estimate=cost(4 * n_tok * rows * units * width, 10 * units * width),
        compiler_params=pltpu.CompilerParams(vmem_limit_bytes=48 * 2**20),
        name="gate_up",
    )(*toks, gate, up, gain, *(near[s] for s in line.swaps), *(far[s] for s in line.swaps))


def down_kernel(line, ks, own, n_tok, *refs):
    swaps = line.swaps
    hidden_ref, refs = refs[0], refs[1:]
    master, refs = refs[0], refs[1:]
    near, refs = dict(zip(swaps, refs)), refs[len(swaps):]
    far, refs = dict(zip(swaps, refs)), refs[len(swaps):]
    if not own:
        refs = refs[1:]
    down_out, refs = refs[0], refs[1:]
    parts, refs = refs[:n_tok], refs[n_tok:]
    held, wide, sem_in, sem_m, sem_out = refs
    g, f = lax.axis_index("grp"), lax.axis_index("fs")
    whole = master.shape[-1]
    half = near[swaps[0]].shape[-1]
    rows = parts[0].shape[0]
    first = 1 if own else 0
    if own:
        mine = pltpu.make_async_copy(master, wide, sem_m)
        mine.start()
    loads = []
    for n, k in enumerate(ks):
        for side, (table, h) in enumerate(((near, g), (far, 1 - g))):
            loads.append(
                slot_loads(
                    line, f, k, table, held.at[first + n, :, at(h * half, half)],
                    sem_in.at[2 * n + side],
                )
            )
    for begin, _ in loads:
        begin()
    places = ([f] if own else []) + [line.piece(f, k) for k in ks]
    stores = [
        pltpu.make_async_copy(held.at[n], down_out.at[:, at(place * whole, whole)], sem_out.at[n])
        for n, place in enumerate(places)
    ]
    for n in range(len(places)):
        if own and n == 0:
            mine.wait()
            held[0] = wide[...].astype(BF16)
        else:
            for _, end in loads[2 * (n - first):2 * (n - first) + 2]:
                end()
        stores[n].start()
        part = jnp.dot(hidden_ref[...], held[n], preferred_element_type=F32).astype(BF16)
        for d in range(n_tok):
            parts[d][:, n * whole:(n + 1) * whole] = part[d * rows:(d + 1) * rows]
    for store in stores:
        store.wait()


def down_part(line, ks, n_tok, hidden, master, near, far, so_far):
    units, whole = master.shape
    width = whole * line.count
    rows = hidden.shape[0] // n_tok
    own = so_far is None
    blocks = len(ks) + (1 if own else 0)
    operands = [hidden, master, *(near[s] for s in line.swaps), *(far[s] for s in line.swaps)]
    in_specs = [VMEM] + [ANY] * (len(operands) - 1)
    aliases = {}
    if not own:
        aliases = {len(operands): 0}
        operands.append(so_far)
        in_specs.append(ANY)
    return pl.pallas_call(
        functools.partial(down_kernel, line, ks, own, n_tok),
        out_shape=(jax.ShapeDtypeStruct((units, width), BF16),)
        + (jax.ShapeDtypeStruct((rows, blocks * whole), BF16),) * n_tok,
        in_specs=in_specs,
        out_specs=(ANY,) + (VMEM,) * n_tok,
        scratch_shapes=[
            pltpu.VMEM((blocks, units, whole), BF16),
            pltpu.VMEM((units, whole), F32),
            pltpu.SemaphoreType.DMA((max(2 * len(ks), 1),)),
            pltpu.SemaphoreType.DMA,
            pltpu.SemaphoreType.DMA((blocks,)),
        ],
        input_output_aliases=aliases,
        cost_estimate=cost(2 * hidden.size * blocks * whole, 4 * units * blocks * whole),
        compiler_params=pltpu.CompilerParams(vmem_limit_bytes=32 * 2**20),
        name="down_first" if own else "down_last",
    )(*operands)


def finish_kernel(line, n_tok, n_parts, tokens_ref, gain_ref, bias_ref, *refs):
    parts = [refs[p * n_tok:(p + 1) * n_tok] for p in range(n_parts)]
    out_ref = refs[n_parts * n_tok]
    f = lax.axis_index("fs")
    width = tokens_ref.shape[-1]
    whole = width // line.count
    places = [f] + [line.piece(f, k) for k in range(line.count - 1)]
    mixed = []
    for p in parts:
        for n in range(p[0].shape[-1] // whole):
            total = p[0][:, n * whole:(n + 1) * whole].astype(F32)
            for other in p[1:]:
                total = total + other[:, n * whole:(n + 1) * whole].astype(F32)
            place = places[len(mixed)]
            wide = tokens_ref[:, at(place * whole, whole)].astype(F32)
            mixed.append(jnp.sqrt(F32(2.0)) * wide + 0.5 * total)
    center = sum(jnp.sum(m, axis=-1, keepdims=True) for m in mixed) / width
    spread = sum(jnp.sum(jnp.square(m - center), axis=-1, keepdims=True) for m in mixed) / width
    scale = lax.rsqrt(spread + 1e-05)
    for place, m in zip(places, mixed):
        cols = at(place * whole, whole)
        out_ref[:, cols] = ((m - center) * scale * gain_ref[:, cols] + bias_ref[:, cols]).astype(BF16)


def finish_all(line, tokens, gain, bias, parts):
    flat = [x for p in parts for x in p]
    return pl.pallas_call(
        functools.partial(finish_kernel, line, len(parts[0]), len(parts)),
        out_shape=jax.ShapeDtypeStruct(tokens.shape, BF16),
        in_specs=[VMEM] * (3 + len(flat)),
        out_specs=VMEM,
        cost_estimate=cost(16 * tokens.size, 16 * tokens.size),
        name="finish",
    )(tokens, gain, bias, *flat)


def over_tp(blocks, n_tok):
    return [blocks[0]] + [
        lax.ppermute(blocks[d], "tp", [(i, i ^ d) for i in range(n_tok)]) for d in range(1, n_tok)
    ]


def exchanged(sizes, tokens, gate_master, up_master, down_master, norm_gain, post_gain, post_bias):
    groups, n_tok = sizes["grp"], sizes["tp"]
    line = Line(sizes["fs"])
    gate, up, down = gate_master.T, up_master.T, down_master.T
    gain = norm_gain[None, :]
    pair_near, pair_far = line_exchange(line, half_pair(gate, up, gain, groups), groups)
    down_near, down_far = line_exchange(line, half_down(down, groups), groups)
    normed = norm(tokens)
    toks = over_tp([normed] * n_tok, n_tok)
    gate_ready, up_ready, hidden = pair(line, toks, gate, up, gain, pair_near, pair_far)
    last = line.count - 2
    down_ready, *first = down_part(
        line, tuple(range(last)), n_tok, hidden, down, down_near, down_far, None
    )
    first = over_tp(first, n_tok)
    down_ready, *rest = down_part(
        line, (last,), n_tok, hidden, down, down_near, down_far, down_ready
    )
    rest = over_tp(rest, n_tok)
    result = finish_all(line, tokens, post_gain[None, :], post_bias[None, :], [first, rest])
    return (gate_ready.T, up_ready.T, down_ready.T, result)


def local(sizes, tokens, gate_master, *rest):
    groups, n_fs, n_tok = sizes["grp"], sizes["fs"], sizes["tp"]
    rows, units = gate_master.shape
    fits = (
        groups == 2
        and 2 < n_fs <= LONGEST_LINE
        and n_tok & (n_tok - 1) == 0
        and rows % (groups * LANES) == 0
        and units % 16 == 0
        and tokens.shape[0] % 16 == 0
    )
    if not fits:
        return plain(tokens, gate_master, *rest)
    return exchanged(sizes, tokens, gate_master, *rest)


def solution(mesh):
    return jax.shard_map(
        functools.partial(local, dict(mesh.shape)),
        mesh=mesh,
        in_specs=(
            P(("grp", "fs", "tp"), None),
            P("fs", "tp"),
            P("fs", "tp"),
            P("fs", "tp"),
            P(),
            P(),
            P(),
        ),
        out_specs=(P("grp", "tp"), P("grp", "tp"), P("grp", "tp"), P(("grp", "fs", "tp"), None)),
        check_vma=False,
    )
```

```python
import functools

import jax
import jax.numpy as jnp
from jax import lax
from jax.experimental import pallas as pl
from jax.experimental.pallas import tpu as pltpu
from jax.sharding import PartitionSpec as P


BF16 = jnp.bfloat16
F32 = jnp.float32
ANY = pl.BlockSpec(memory_space=pl.ANY)
VMEM = pl.BlockSpec(memory_space=pltpu.VMEM)
LANES = 128
LONGEST_LINE = 8


def finish(wide, branch, post_gain, post_bias):
    mixed = jnp.sqrt(jnp.float32(2.0)) * wide + 0.5 * branch
    center = jnp.mean(mixed, axis=-1, keepdims=True)
    spread = jnp.mean(jnp.square(mixed - center), axis=-1, keepdims=True)
    return ((mixed - center) * lax.rsqrt(spread + 1e-05) * post_gain + post_bias).astype(
        jnp.bfloat16
    )


def plain(tokens, gate_master, up_master, down_master, norm_gain, post_gain, post_bias):
    row_count = gate_master.shape[0]
    first_row = lax.axis_index("fs") * row_count
    gain_rows = lax.dynamic_slice_in_dim(norm_gain, first_row, row_count, 0)
    gate_piece = (gain_rows[:, None] * gate_master).astype(BF16)
    up_piece = (gain_rows[:, None] * up_master).astype(BF16)
    down_piece = down_master.astype(BF16)
    gate_ready, up_ready, down_ready = (
        lax.all_gather(gate_piece, "fs", axis=0, tiled=True),
        lax.all_gather(up_piece, "fs", axis=0, tiled=True),
        lax.all_gather(down_piece, "fs", axis=0, tiled=True),
    )
    wide = tokens.astype(F32)
    normed = (wide * lax.rsqrt(jnp.mean(wide * wide, axis=-1, keepdims=True) + 1e-06)).astype(BF16)
    piece = lax.all_gather(normed, "tp", axis=0, tiled=True)
    gate = jnp.dot(piece, gate_ready, preferred_element_type=F32)
    upward = jnp.dot(piece, up_ready, preferred_element_type=F32)
    hidden = (jax.nn.silu(gate) * upward).astype(BF16)
    branch = lax.psum_scatter(
        lax.dot_general(
            hidden, down_ready, (((1,), (1,)), ((), ())), preferred_element_type=F32
        ).astype(BF16),
        "tp",
        scatter_dimension=0,
        tiled=True,
    ).astype(F32)
    return (gate_ready, up_ready, down_ready, finish(wide, branch, post_gain, post_bias))


class Line:
    def __init__(self, count):
        self.count = count
        self.swaps = []
        self.pairs = {}
        self.brings = {}
        for t in range(1, count):
            for q in (0, 1):
                pairs, brings = [], {}
                for i in range(q, count - 1, 2):
                    if i - t + 1 >= 0:
                        pairs.append((i, i + 1))
                        brings[i + 1] = i + 1 - t
                    if i + t < count:
                        pairs.append((i + 1, i))
                        brings[i] = i + t
                if pairs:
                    self.swaps.append((t, q))
                    self.pairs[t, q] = pairs
                    self.brings[t, q] = brings
        self.order = {f: [s for s in self.swaps if f in self.brings[s]] for f in range(count)}
        self.slots = [
            sorted({self.order[f][k] for f in range(count)}) for k in range(count - 1)
        ]

    def piece(self, f, k):
        out = jnp.int32(0)
        for i in range(self.count):
            s = self.order[i][k]
            out = jnp.where(f == i, jnp.int32(self.brings[s][i]), out)
        return out

    def holds(self, f, k, s):
        out = f < 0
        for i in range(self.count):
            if self.order[i][k] == s:
                out = jnp.logical_or(out, f == i)
        return out


def line_exchange(line, half, groups):
    near, far = {}, {}
    for t, q in line.swaps:
        operand = half if t == 1 else near[t - 1, 1 - q]
        near[t, q] = lax.ppermute(operand, "fs", line.pairs[t, q])
        across = [
            (g * line.count + f, ((g + 1) % groups) * line.count + f)
            for g in range(groups)
            for f in line.brings[t, q]
        ]
        far[t, q] = lax.ppermute(near[t, q], ("grp", "fs"), across)
    return near, far


def at(start, size):
    return pl.ds(pl.multiple_of(start, LANES), size)


def cost(flops, moved):
    return pl.CostEstimate(flops=flops, bytes_accessed=moved, transcendentals=0)


def half_kernel(scaled, *refs):
    if scaled:
        master_ref, gain_ref, out_ref, buf, sem = refs
    else:
        master_ref, out_ref, buf, sem = refs
    half = out_ref.shape[-1]
    whole = master_ref.shape[-1]
    g, f = lax.axis_index("grp"), lax.axis_index("fs")
    load = pltpu.make_async_copy(master_ref.at[:, at(g * half, half)], buf, sem)
    load.start()
    load.wait()
    value = buf[...]
    if scaled:
        value = value * gain_ref[:, at(f * whole + g * half, half)]
    out_ref[...] = value.astype(BF16)


def half_piece(groups, master, gain=None):
    units, whole = master.shape
    half = whole // groups
    operands = [master] if gain is None else [master, gain]
    return pl.pallas_call(
        functools.partial(half_kernel, gain is not None),
        out_shape=jax.ShapeDtypeStruct((units, half), BF16),
        in_specs=[ANY, VMEM][: len(operands)],
        out_specs=VMEM,
        scratch_shapes=[pltpu.VMEM((units, half), F32), pltpu.SemaphoreType.DMA],
        cost_estimate=cost(units * half, 6 * units * half),
        compiler_params=pltpu.CompilerParams(vmem_limit_bytes=8 * 2**20),
        name="half_piece",
    )(*operands)


def norm_kernel(tokens_ref, out_ref):
    wide = tokens_ref[...].astype(F32)
    scale = lax.rsqrt(jnp.mean(wide * wide, axis=-1, keepdims=True) + 1e-06)
    out_ref[...] = (wide * scale).astype(BF16)


def norm(tokens):
    return pl.pallas_call(
        norm_kernel,
        out_shape=jax.ShapeDtypeStruct(tokens.shape, BF16),
        in_specs=[VMEM],
        out_specs=VMEM,
        cost_estimate=cost(4 * tokens.size, 4 * tokens.size),
        compiler_params=pltpu.CompilerParams(vmem_limit_bytes=8 * 2**20),
        name="norm_tokens",
    )(tokens)


def slot_loads(line, f, k, refs, fill, sem):
    swaps = line.slots[k]

    def each(act):
        for s in swaps:
            if len(swaps) == 1:
                act(pltpu.make_async_copy(refs[s], fill, sem))
            else:

                @pl.when(line.holds(f, k, s))
                def _():
                    act(pltpu.make_async_copy(refs[s], fill, sem))

    return (lambda: each(lambda c: c.start())), (lambda: each(lambda c: c.wait()))


def taken(line, ks):
    return sorted({s for k in ks for s in line.slots[k]})


def split(refs, *counts):
    out = []
    for n in counts:
        out.append(refs[:n])
        refs = refs[n:]
    return (*out, refs)


def pair_kernel(line, ks, own, n_tok, *refs):
    swaps = taken(line, ks)
    toks, refs = split(refs, n_tok)
    tables = []
    for _ in range(4):
        some, refs = split(refs, len(swaps))
        tables.append(dict(zip(swaps, some)))
    if own:
        (gate_ref, up_ref, gain_ref), refs = split(refs, 3)
    else:
        (so_far, _, _), refs = split(refs, 3)
    gate_out, up_out, out_ref, normed, held, masters, sem_in, sem_m, sem_t, sem_out = refs
    g, f = lax.axis_index("grp"), lax.axis_index("fs")
    whole = toks[0].shape[-1] // line.count
    half = tables[0][swaps[0]].shape[-1]
    rows = toks[0].shape[0]
    first = 1 if own else 0
    places = ([f] if own else []) + [line.piece(f, k) for k in ks]
    mine = []
    if own:
        mine = [
            pltpu.make_async_copy(src, masters.at[n], sem_m.at[n])
            for n, src in enumerate((gate_ref, up_ref))
        ]
    for load in mine:
        load.start()
    loads = []
    for i, k in enumerate(ks):
        for n, table in enumerate(tables):
            h = 1 - g if n % 2 else g
            fill = held.at[n // 2, :, at((first + i) * whole + h * half, half)]
            loads.append(slot_loads(line, f, k, table, fill, sem_in.at[4 * i + n]))
    token_loads = [
        pltpu.make_async_copy(
            tok.at[:, at(place * whole, whole)],
            normed.at[pl.ds(d * rows, rows), pl.ds(i * whole, whole)],
            sem_t.at[d * len(places) + i],
        )
        for d, tok in enumerate(toks)
        for i, place in enumerate(places)
    ]
    for load in token_loads:
        load.start()
    for begin, _ in loads:
        begin()
    stores = [
        [
            pltpu.make_async_copy(
                held.at[n, :, pl.ds(i * whole, whole)],
                out.at[:, at(place * whole, whole)],
                sem_out.at[2 * i + n],
            )
            for n, out in enumerate((gate_out, up_out))
        ]
        for i, place in enumerate(places)
    ]
    if own:
        gain = gain_ref[:, at(f * whole, whole)]
        for n, load in enumerate(mine):
            load.wait()
            held[n, :, :whole] = (masters[n] * gain).astype(BF16)
            stores[0][n].start()
    for i in range(len(ks)):
        for _, end in loads[4 * i:4 * i + 4]:
            end()
        for store in stores[first + i]:
            store.start()
    for load in token_loads:
        load.wait()
    gate, up = [
        lax.dot_general(
            normed[...], held[n], (((1,), (1,)), ((), ())), preferred_element_type=F32
        )
        for n in range(2)
    ]
    if own:
        out_ref[0] = gate
        out_ref[1] = up
    else:
        gate = gate + so_far[0]
        up = up + so_far[1]
        out_ref[...] = (gate / (1.0 + jnp.exp(-gate)) * up).astype(BF16)
    for some in stores:
        for store in some:
            store.wait()


def pair_part(line, ks, toks, tables, masters, so_far):
    own = so_far is None
    rows, width = toks[0].shape
    whole = width // line.count
    n_tok = len(toks)
    swaps = taken(line, ks)
    units = tables[0][swaps[0]].shape[0]
    blocks = len(ks) + (1 if own else 0)
    operands = [*toks, *(table[s] for table in tables for s in swaps)]
    in_specs = [ANY] * len(operands)
    aliases = {}
    if own:
        operands += masters
        in_specs += [ANY, ANY, VMEM]
        last = jax.ShapeDtypeStruct((2, n_tok * rows, units), F32)
    else:
        aliases = {len(operands) + 1: 0, len(operands) + 2: 1}
        operands += so_far
        in_specs += [VMEM, ANY, ANY]
        last = jax.ShapeDtypeStruct((n_tok * rows, units), BF16)
    ready = jax.ShapeDtypeStruct((units, width), BF16)
    return pl.pallas_call(
        functools.partial(pair_kernel, line, ks, own, n_tok),
        out_shape=(ready, ready, last),
        in_specs=in_specs,
        out_specs=(ANY, ANY, VMEM),
        scratch_shapes=[
            pltpu.VMEM((n_tok * rows, blocks * whole), BF16),
            pltpu.VMEM((2, units, blocks * whole), BF16),
            pltpu.VMEM((2, units, whole), F32),
            pltpu.SemaphoreType.DMA((4 * len(ks),)),
            pltpu.SemaphoreType.DMA((2,)),
            pltpu.SemaphoreType.DMA((n_tok * blocks,)),
            pltpu.SemaphoreType.DMA((2 * blocks,)),
        ],
        input_output_aliases=aliases,
        cost_estimate=cost(4 * n_tok * rows * units * blocks * whole, 10 * units * blocks * whole),
        compiler_params=pltpu.CompilerParams(vmem_limit_bytes=24 * 2**20),
        name="pair_first" if own else "pair_last",
    )(*operands)


def down_kernel(line, ks, own, n_tok, *refs):
    swaps = taken(line, ks)
    (hidden_ref, extra), near, far, refs = split(refs, 2, len(swaps), len(swaps))
    near, far = dict(zip(swaps, near)), dict(zip(swaps, far))
    down_out, refs = refs[0], refs[1:]
    parts, refs = split(refs, n_tok)
    held, wide, sem_in, sem_m, sem_out = refs
    g, f = lax.axis_index("grp"), lax.axis_index("fs")
    whole = wide.shape[-1]
    half = near[swaps[0]].shape[-1]
    rows = parts[0].shape[0]
    first = 1 if own else 0
    if own:
        mine = pltpu.make_async_copy(extra, wide, sem_m)
        mine.start()
    loads = []
    for n, k in enumerate(ks):
        for side, (table, h) in enumerate(((near, g), (far, 1 - g))):
            loads.append(
                slot_loads(
                    line, f, k, table, held.at[first + n, :, at(h * half, half)],
                    sem_in.at[2 * n + side],
                )
            )
    for begin, _ in loads:
        begin()
    places = ([f] if own else []) + [line.piece(f, k) for k in ks]
    stores = [
        pltpu.make_async_copy(held.at[n], down_out.at[:, at(place * whole, whole)], sem_out.at[n])
        for n, place in enumerate(places)
    ]
    for n in range(len(places)):
        if own and n == 0:
            mine.wait()
            held[0] = wide[...].astype(BF16)
        else:
            for _, end in loads[2 * (n - first):2 * (n - first) + 2]:
                end()
        stores[n].start()
        part = jnp.dot(hidden_ref[...], held[n], preferred_element_type=F32).astype(BF16)
        for d in range(n_tok):
            parts[d][:, n * whole:(n + 1) * whole] = part[d * rows:(d + 1) * rows]
    for store in stores:
        store.wait()


def down_part(line, ks, n_tok, whole, hidden, near, far, master, so_far):
    units = hidden.shape[1]
    width = whole * line.count
    rows = hidden.shape[0] // n_tok
    own = so_far is None
    blocks = len(ks) + (1 if own else 0)
    swaps = taken(line, ks)
    operands = [
        hidden, master if own else so_far, *(near[s] for s in swaps), *(far[s] for s in swaps)
    ]
    return pl.pallas_call(
        functools.partial(down_kernel, line, ks, own, n_tok),
        out_shape=(jax.ShapeDtypeStruct((units, width), BF16),)
        + (jax.ShapeDtypeStruct((rows, blocks * whole), BF16),) * n_tok,
        in_specs=[VMEM] + [ANY] * (len(operands) - 1),
        out_specs=(ANY,) + (VMEM,) * n_tok,
        scratch_shapes=[
            pltpu.VMEM((blocks, units, whole), BF16),
            pltpu.VMEM((units, whole), F32),
            pltpu.SemaphoreType.DMA((2 * len(ks),)),
            pltpu.SemaphoreType.DMA,
            pltpu.SemaphoreType.DMA((blocks,)),
        ],
        input_output_aliases={} if own else {1: 0},
        cost_estimate=cost(2 * hidden.size * blocks * whole, 4 * units * blocks * whole),
        compiler_params=pltpu.CompilerParams(vmem_limit_bytes=12 * 2**20),
        name="down_first" if own else "down_last",
    )(*operands)


def finish_kernel(line, widths, n_tok, *refs):
    n_parts = len(widths)
    parts, refs = refs[:n_parts * n_tok], refs[n_parts * n_tok:]
    tokens_ref, gain_ref, bias_ref, out_ref = refs[:4]
    bufs, sem = refs[4:4 + n_parts], refs[4 + n_parts]
    loads = [
        pltpu.make_async_copy(parts[p * n_tok + d], bufs[p].at[d], sem.at[p * n_tok + d])
        for p in range(n_parts)
        for d in range(n_tok)
    ]
    for load in loads:
        load.start()
    f = lax.axis_index("fs")
    width = tokens_ref.shape[-1]
    whole = width // line.count
    places = [f] + [line.piece(f, k) for k in range(line.count - 1)]
    mixed = []
    for p in range(n_parts):
        for load in loads[p * n_tok:(p + 1) * n_tok]:
            load.wait()
        for n in range(widths[p] // whole):
            total = bufs[p][0, :, n * whole:(n + 1) * whole].astype(F32)
            for d in range(1, n_tok):
                total = total + bufs[p][d, :, n * whole:(n + 1) * whole].astype(F32)
            wide = tokens_ref[:, at(places[len(mixed)] * whole, whole)].astype(F32)
            mixed.append(jnp.sqrt(F32(2.0)) * wide + 0.5 * total)
    center = sum(jnp.sum(m, axis=-1, keepdims=True) for m in mixed) / width
    spread = sum(jnp.sum(jnp.square(m - center), axis=-1, keepdims=True) for m in mixed) / width
    scale = lax.rsqrt(spread + 1e-05)
    for place, m in zip(places, mixed):
        cols = at(place * whole, whole)
        out_ref[:, cols] = ((m - center) * scale * gain_ref[:, cols] + bias_ref[:, cols]).astype(BF16)


def finish_all(line, tokens, gain, bias, parts):
    flat = [x for p in parts for x in p]
    n_tok = len(parts[0])
    widths = tuple(p[0].shape[-1] for p in parts)
    return pl.pallas_call(
        functools.partial(finish_kernel, line, widths, n_tok),
        out_shape=jax.ShapeDtypeStruct(tokens.shape, BF16),
        in_specs=[ANY] * len(flat) + [VMEM] * 3,
        out_specs=VMEM,
        scratch_shapes=[pltpu.VMEM((n_tok, tokens.shape[0], w), BF16) for w in widths]
        + [pltpu.SemaphoreType.DMA((len(flat),))],
        cost_estimate=cost(16 * tokens.size, 16 * tokens.size),
        compiler_params=pltpu.CompilerParams(vmem_limit_bytes=8 * 2**20),
        name="finish",
    )(*flat, tokens, gain, bias)


def over_tp(blocks, n_tok):
    return [blocks[0]] + [
        lax.ppermute(blocks[d], "tp", [(i, i ^ d) for i in range(n_tok)])
        for d in range(1, n_tok)
    ]


def exchanged(sizes, tokens, gate_master, up_master, down_master, norm_gain, post_gain, post_bias):
    groups, n_tok = sizes["grp"], sizes["tp"]
    line = Line(sizes["fs"])
    gate, up, down = gate_master.T, up_master.T, down_master.T
    gain = norm_gain[None, :]
    last = line.count - 2
    head = tuple(range(last))

    tables = []
    for operands in ((gate, gain), (up, gain), (down,)):
        half = half_piece(groups, *operands)
        tables += line_exchange(line, half, groups)
    pair_tables, (near, far) = tables[:4], tables[4:]
    toks = over_tp([norm(tokens)] * n_tok, n_tok)
    gate_ready, up_ready, so_far = pair_part(line, head, toks, pair_tables, [gate, up, gain], None)
    gate_ready, up_ready, hidden = pair_part(
        line, (last,), toks, pair_tables, None,
        [so_far, gate_ready, up_ready],
    )
    whole = down.shape[1]
    down_ready, *first = down_part(line, head, n_tok, whole, hidden, near, far, down, None)
    first = over_tp(first, n_tok)
    down_ready, *rest = down_part(line, (last,), n_tok, whole, hidden, near, far, None, down_ready)
    rest = over_tp(rest, n_tok)
    result = finish_all(line, tokens, post_gain[None, :], post_bias[None, :], [first, rest])
    return (gate_ready.T, up_ready.T, down_ready.T, result)


def fits(sizes, tokens, gate_master):
    groups, n_fs, n_tok = sizes["grp"], sizes["fs"], sizes["tp"]
    rows = gate_master.shape[0] // n_fs
    units = gate_master.shape[1] // n_tok
    return (
        groups == 2
        and 2 < n_fs <= LONGEST_LINE
        and n_tok & (n_tok - 1) == 0
        and rows % (groups * LANES) == 0
        and units % 16 == 0
        and tokens.shape[0] // (groups * n_fs * n_tok) % 16 == 0
    )


def solution(mesh):
    sizes = dict(mesh.shape)
    rows = P(("grp", "fs", "tp"), None)
    ready = P("grp", "tp")

    def over_mesh(body):
        return jax.shard_map(
            body,
            mesh=mesh,
            in_specs=(rows, P("fs", "tp"), P("fs", "tp"), P("fs", "tp"), P(), P(), P()),
            out_specs=(ready, ready, ready, rows),
            check_vma=False,
        )

    def run(tokens, gate_master, *rest):
        if not fits(sizes, tokens, gate_master):
            return over_mesh(plain)(tokens, gate_master, *rest)
        step = over_mesh(functools.partial(exchanged, sizes))
        return step(tokens, gate_master, *rest)

    return run
```

```python
import functools

import jax
import jax.numpy as jnp
from jax import lax
from jax.experimental import pallas as pl
from jax.experimental.pallas import tpu as pltpu
from jax.sharding import PartitionSpec as P


BF16 = jnp.bfloat16
F32 = jnp.float32
ANY = pl.BlockSpec(memory_space=pl.ANY)
VMEM = pl.BlockSpec(memory_space=pltpu.VMEM)
LANES = 128
LONGEST_LINE = 8


def finish(wide, branch, post_gain, post_bias):
    mixed = jnp.sqrt(jnp.float32(2.0)) * wide + 0.5 * branch
    center = jnp.mean(mixed, axis=-1, keepdims=True)
    spread = jnp.mean(jnp.square(mixed - center), axis=-1, keepdims=True)
    return ((mixed - center) * lax.rsqrt(spread + 1e-05) * post_gain + post_bias).astype(
        jnp.bfloat16
    )


def plain(tokens, gate_master, up_master, down_master, norm_gain, post_gain, post_bias):
    row_count = gate_master.shape[0]
    first_row = lax.axis_index("fs") * row_count
    gain_rows = lax.dynamic_slice_in_dim(norm_gain, first_row, row_count, 0)
    gate_piece = (gain_rows[:, None] * gate_master).astype(BF16)
    up_piece = (gain_rows[:, None] * up_master).astype(BF16)
    down_piece = down_master.astype(BF16)
    gate_ready, up_ready, down_ready = (
        lax.all_gather(gate_piece, "fs", axis=0, tiled=True),
        lax.all_gather(up_piece, "fs", axis=0, tiled=True),
        lax.all_gather(down_piece, "fs", axis=0, tiled=True),
    )
    wide = tokens.astype(F32)
    normed = (wide * lax.rsqrt(jnp.mean(wide * wide, axis=-1, keepdims=True) + 1e-06)).astype(BF16)
    piece = lax.all_gather(normed, "tp", axis=0, tiled=True)
    gate = jnp.dot(piece, gate_ready, preferred_element_type=F32)
    upward = jnp.dot(piece, up_ready, preferred_element_type=F32)
    hidden = (jax.nn.silu(gate) * upward).astype(BF16)
    branch = lax.psum_scatter(
        lax.dot_general(
            hidden, down_ready, (((1,), (1,)), ((), ())), preferred_element_type=F32
        ).astype(BF16),
        "tp",
        scatter_dimension=0,
        tiled=True,
    ).astype(F32)
    return (gate_ready, up_ready, down_ready, finish(wide, branch, post_gain, post_bias))


class Line:
    def __init__(self, count):
        self.count = count
        self.swaps = []
        self.pairs = {}
        self.brings = {}
        for t in range(1, count):
            for q in (0, 1):
                pairs, brings = [], {}
                for i in range(q, count - 1, 2):
                    if i - t + 1 >= 0:
                        pairs.append((i, i + 1))
                        brings[i + 1] = i + 1 - t
                    if i + t < count:
                        pairs.append((i + 1, i))
                        brings[i] = i + t
                if pairs:
                    self.swaps.append((t, q))
                    self.pairs[t, q] = pairs
                    self.brings[t, q] = brings
        self.order = {f: [s for s in self.swaps if f in self.brings[s]] for f in range(count)}
        self.slots = [
            sorted({self.order[f][k] for f in range(count)}) for k in range(count - 1)
        ]

    def piece(self, f, k):
        out = jnp.int32(0)
        for i in range(self.count):
            s = self.order[i][k]
            out = jnp.where(f == i, jnp.int32(self.brings[s][i]), out)
        return out

    def holds(self, f, k, s):
        out = f < 0
        for i in range(self.count):
            if self.order[i][k] == s:
                out = jnp.logical_or(out, f == i)
        return out


MESH = ("grp", "fs", "tp")


def whole_moves(sizes, step):
    groups, n_fs, n_tok = (sizes[axis] for axis in MESH)

    def index(g, f, t):
        return (g * n_fs + f) * n_tok + t

    moves = []
    for g in range(groups):
        for f in range(n_fs):
            to = step(g, f)
            for t in range(n_tok):
                target = index(g, f, t ^ 1) if to is None else index(*to, t)
                moves.append((index(g, f, t), target))
    return moves


def line_exchange(line, halves, sizes):
    near, far = {}, {}
    for t, q in line.swaps:
        ends = {i for pair in line.pairs[t, q] for i in pair}

        def along(g, f):
            return (g, f + 1 if f % 2 == q else f - 1) if f in ends else None

        def across(g, f):
            return ((g + 1) % sizes["grp"], f) if f in line.brings[t, q] else None

        operand = halves[0] if t == 1 else near[t - 1, 1 - q]
        near[t, q] = lax.ppermute(operand, MESH, whole_moves(sizes, along))
        if t == 1 and len(halves) > 1:
            far[t, q] = lax.ppermute(halves[1], MESH, whole_moves(sizes, along))
        else:
            far[t, q] = lax.ppermute(near[t, q], MESH, whole_moves(sizes, across))
    return near, far


def at(start, size):
    return pl.ds(pl.multiple_of(start, LANES), size)


def cost(flops, moved):
    return pl.CostEstimate(flops=flops, bytes_accessed=moved, transcendentals=0)


def half_kernel(groups, cuts, *refs):
    *operands, buf, sem = refs
    master_ref, outs = operands[0], operands[-len(cuts):]
    whole = master_ref.shape[-1]
    width = outs[0].shape[-1]
    g, f = lax.axis_index("grp"), lax.axis_index("fs")
    starts = [(1 - g if side else g) * (whole // groups) + n * width for side, n in cuts]
    loads = [
        pltpu.make_async_copy(master_ref.at[:, at(start, width)], buf.at[n], sem.at[n])
        for n, start in enumerate(starts)
    ]
    for load in loads:
        load.start()
    for n, load in enumerate(loads):
        load.wait()
        value = buf[n]
        if len(operands) > len(cuts) + 1:
            value = value * operands[1][:, at(f * whole + starts[n], width)]
        outs[n][...] = value.astype(BF16)


def half_pieces(groups, width, cuts, master, gain=None):
    units = master.shape[0]
    count = len(cuts)
    operands = [master] if gain is None else [master, gain]
    return pl.pallas_call(
        functools.partial(half_kernel, groups, cuts),
        out_shape=(jax.ShapeDtypeStruct((units, width), BF16),) * count,
        in_specs=[ANY, VMEM][: len(operands)],
        out_specs=(VMEM,) * count,
        scratch_shapes=[
            pltpu.VMEM((count, units, width), F32),
            pltpu.SemaphoreType.DMA((count,)),
        ],
        cost_estimate=cost(2**32, 6 * units * width * count),
        compiler_params=pltpu.CompilerParams(vmem_limit_bytes=8 * 2**20),
        name="half_pieces",
    )(*operands)


def norm_kernel(tokens_ref, out_ref):
    wide = tokens_ref[...].astype(F32)
    scale = lax.rsqrt(jnp.mean(wide * wide, axis=-1, keepdims=True) + 1e-06)
    out_ref[...] = (wide * scale).astype(BF16)


def norm(tokens):
    return pl.pallas_call(
        norm_kernel,
        out_shape=jax.ShapeDtypeStruct(tokens.shape, BF16),
        in_specs=[VMEM],
        out_specs=VMEM,
        cost_estimate=cost(4 * tokens.size, 4 * tokens.size),
        compiler_params=pltpu.CompilerParams(vmem_limit_bytes=8 * 2**20),
        name="norm_tokens",
    )(tokens)


def slot_loads(line, f, k, refs, fill, sem):
    swaps = line.slots[k]

    def each(act):
        for s in swaps:
            if len(swaps) == 1:
                act(pltpu.make_async_copy(refs[s], fill, sem))
            else:

                @pl.when(line.holds(f, k, s))
                def _():
                    act(pltpu.make_async_copy(refs[s], fill, sem))

    return (lambda: each(lambda c: c.start())), (lambda: each(lambda c: c.wait()))


def taken(line, ks):
    return sorted({s for k in ks for s in line.slots[k]})


def split(refs, *counts):
    out = []
    for n in counts:
        out.append(refs[:n])
        refs = refs[n:]
    return (*out, refs)


def pair_kernel(line, ks, own, n_tok, *refs):
    swaps = taken(line, ks)
    toks, refs = split(refs, n_tok)
    tables = []
    for _ in range(4):
        some, refs = split(refs, len(swaps))
        tables.append(dict(zip(swaps, some)))
    if own:
        (gate_ref, up_ref, gain_ref), refs = split(refs, 3)
    else:
        (so_far, _, _), refs = split(refs, 3)
    gate_out, up_out, out_ref, normed, held, masters, sem_in, sem_m, sem_t, sem_out = refs
    g, f = lax.axis_index("grp"), lax.axis_index("fs")
    whole = toks[0].shape[-1] // line.count
    half = tables[0][swaps[0]].shape[-1]
    rows = toks[0].shape[0]
    first = 1 if own else 0
    places = ([f] if own else []) + [line.piece(f, k) for k in ks]
    mine = []
    if own:
        mine = [
            pltpu.make_async_copy(src, masters.at[n], sem_m.at[n])
            for n, src in enumerate((gate_ref, up_ref))
        ]
    for load in mine:
        load.start()
    loads = []
    for i, k in enumerate(ks):
        for n, table in enumerate(tables):
            h = 1 - g if n % 2 else g
            fill = held.at[n // 2, :, at((first + i) * whole + h * half, half)]
            loads.append(slot_loads(line, f, k, table, fill, sem_in.at[4 * i + n]))
    token_loads = [
        pltpu.make_async_copy(
            tok.at[:, at(place * whole, whole)],
            normed.at[pl.ds(d * rows, rows), pl.ds(i * whole, whole)],
            sem_t.at[d * len(places) + i],
        )
        for d, tok in enumerate(toks)
        for i, place in enumerate(places)
    ]
    for load in token_loads:
        load.start()
    for begin, _ in loads:
        begin()
    stores = [
        [
            pltpu.make_async_copy(
                held.at[n, :, pl.ds(i * whole, whole)],
                out.at[:, at(place * whole, whole)],
                sem_out.at[2 * i + n],
            )
            for n, out in enumerate((gate_out, up_out))
        ]
        for i, place in enumerate(places)
    ]
    if own:
        gain = gain_ref[:, at(f * whole, whole)]
        for n, load in enumerate(mine):
            load.wait()
            held[n, :, :whole] = (masters[n] * gain).astype(BF16)
            stores[0][n].start()
    for i in range(len(ks)):
        for _, end in loads[4 * i:4 * i + 4]:
            end()
        for store in stores[first + i]:
            store.start()
    for load in token_loads:
        load.wait()
    gate, up = [
        lax.dot_general(
            normed[...], held[n], (((1,), (1,)), ((), ())), preferred_element_type=F32
        )
        for n in range(2)
    ]
    if own:
        out_ref[0] = gate
        out_ref[1] = up
    else:
        gate = gate + so_far[0]
        up = up + so_far[1]
        out_ref[...] = (gate / (1.0 + jnp.exp(-gate)) * up).astype(BF16)
    for some in stores:
        for store in some:
            store.wait()


def pair_part(line, ks, toks, tables, masters, so_far):
    own = so_far is None
    rows, width = toks[0].shape
    whole = width // line.count
    n_tok = len(toks)
    swaps = taken(line, ks)
    units = tables[0][swaps[0]].shape[0]
    blocks = len(ks) + (1 if own else 0)
    operands = [*toks, *(table[s] for table in tables for s in swaps)]
    in_specs = [ANY] * len(operands)
    aliases = {}
    if own:
        operands += masters
        in_specs += [ANY, ANY, VMEM]
        last = jax.ShapeDtypeStruct((2, n_tok * rows, units), F32)
    else:
        aliases = {len(operands) + 1: 0, len(operands) + 2: 1}
        operands += so_far
        in_specs += [VMEM, ANY, ANY]
        last = jax.ShapeDtypeStruct((n_tok * rows, units), BF16)
    ready = jax.ShapeDtypeStruct((units, width), BF16)
    return pl.pallas_call(
        functools.partial(pair_kernel, line, ks, own, n_tok),
        out_shape=(ready, ready, last),
        in_specs=in_specs,
        out_specs=(ANY, ANY, VMEM),
        scratch_shapes=[
            pltpu.VMEM((n_tok * rows, blocks * whole), BF16),
            pltpu.VMEM((2, units, blocks * whole), BF16),
            pltpu.VMEM((2, units, whole), F32),
            pltpu.SemaphoreType.DMA((4 * len(ks),)),
            pltpu.SemaphoreType.DMA((2,)),
            pltpu.SemaphoreType.DMA((n_tok * blocks,)),
            pltpu.SemaphoreType.DMA((2 * blocks,)),
        ],
        input_output_aliases=aliases,
        cost_estimate=cost(4 * n_tok * rows * units * blocks * whole, 10 * units * blocks * whole),
        compiler_params=pltpu.CompilerParams(vmem_limit_bytes=24 * 2**20),
        name="pair_first" if own else "pair_last",
    )(*operands)


OWN = -1


class Blocks:
    def __init__(self, line, groups, whole, cut):
        self.line, self.groups, self.whole, self.cut = line, groups, whole, cut

    def width(self, block):
        return self.whole if block[0] == OWN else self.cut

    def widths(self, blocks):
        return sum(self.width(block) for block in blocks)

    def spans(self, blocks):
        n = 0
        for block in blocks:
            yield block, n, self.width(block)
            n += self.width(block)

    def column(self, block):
        g, f = lax.axis_index("grp"), lax.axis_index("fs")
        if block[0] == OWN:
            return f * self.whole
        k, side, n = block
        half = (1 - g if side else g) * (self.whole // self.groups)
        return self.line.piece(f, k) * self.whole + half + n * self.cut

    def sources(self, blocks):
        return sorted(
            {(b[1], b[2], s) for b in blocks if b[0] != OWN for s in self.line.slots[b[0]]}
        )

    def operands(self, blocks, tables):
        return [tables[n][side][s] for side, n, s in self.sources(blocks)]

    def loads(self, blocks, refs, held, sem):
        f = lax.axis_index("fs")
        named = dict(zip(self.sources(blocks), refs))
        waits = []
        for i, (block, start, width) in enumerate(self.spans(blocks)):
            if block[0] == OWN:
                continue
            k, side, n = block
            table = {s: named[side, n, s] for s in self.line.slots[k]}
            begin, end = slot_loads(
                self.line, f, k, table, held.at[:, pl.ds(start, width)], sem.at[i]
            )
            begin()
            waits.append(end)
        return waits

    def stores(self, blocks, held, out, sem):
        return [
            pltpu.make_async_copy(
                held.at[:, pl.ds(start, width)], out.at[:, at(self.column(block), width)], sem.at[i]
            )
            for i, (block, start, width) in enumerate(self.spans(blocks))
        ]


def multiply(hidden_ref, held, start, stop, parts):
    rows = parts[0].shape[0]
    part = jnp.dot(
        hidden_ref[...], held[:, start:stop], preferred_element_type=F32
    ).astype(BF16)
    for d, ref in enumerate(parts):
        ref[:, start:stop] = part[d * rows:(d + 1) * rows]


def down_own_kernel(form, blocks, n_tok, *refs):
    count = len(form.sources(blocks))
    (hidden_ref, master), some, (down_out,), parts, scratch = split(refs, 2, count, 1, n_tok)
    held, wide, sem_in, sem_m, sem_out = scratch
    mine = pltpu.make_async_copy(master, wide, sem_m)
    mine.start()
    waits = form.loads(blocks, some, held, sem_in)
    first, *others = form.stores(blocks, held, down_out, sem_out)
    mine.wait()
    held[:, :form.whole] = wide[...].astype(BF16)
    first.start()
    multiply(hidden_ref, held, 0, form.whole, parts)
    for wait in waits:
        wait()
    for store in others:
        store.start()
    multiply(hidden_ref, held, form.whole, form.widths(blocks), parts)
    for store in (first, *others):
        store.wait()


def down_own(form, blocks, n_tok, hidden, tables, master):
    some = form.operands(blocks, tables)
    units = master.shape[0]
    rows = hidden.shape[0] // n_tok
    width = form.widths(blocks)
    return pl.pallas_call(
        functools.partial(down_own_kernel, form, blocks, n_tok),
        out_shape=(jax.ShapeDtypeStruct((units, form.whole * form.line.count), BF16),)
        + (jax.ShapeDtypeStruct((rows, width), BF16),) * n_tok,
        in_specs=[VMEM] + [ANY] * (len(some) + 1),
        out_specs=(ANY,) + (VMEM,) * n_tok,
        scratch_shapes=[
            pltpu.VMEM((units, width), BF16),
            pltpu.VMEM((units, form.whole), F32),
            pltpu.SemaphoreType.DMA((len(blocks),)),
            pltpu.SemaphoreType.DMA,
            pltpu.SemaphoreType.DMA((len(blocks),)),
        ],
        cost_estimate=cost(2 * hidden.size * width, 4 * units * width),
        compiler_params=pltpu.CompilerParams(vmem_limit_bytes=12 * 2**20),
        name="down_own",
    )(hidden, master, *some)


def down_more_kernel(form, blocks, n_tok, *refs):
    (hidden_ref,), some, parts, (held, sem_in) = split(refs, 1, len(form.sources(blocks)), n_tok)
    for wait in form.loads(blocks, some, held, sem_in):
        wait()
    multiply(hidden_ref, held, 0, form.widths(blocks), parts)


def down_more(form, blocks, n_tok, hidden, tables):
    some = form.operands(blocks, tables)
    units = hidden.shape[1]
    rows = hidden.shape[0] // n_tok
    width = form.widths(blocks)
    return pl.pallas_call(
        functools.partial(down_more_kernel, form, blocks, n_tok),
        out_shape=(jax.ShapeDtypeStruct((rows, width), BF16),) * n_tok,
        in_specs=[VMEM] + [ANY] * len(some),
        out_specs=(VMEM,) * n_tok,
        scratch_shapes=[
            pltpu.VMEM((units, width), BF16),
            pltpu.SemaphoreType.DMA((len(blocks),)),
        ],
        cost_estimate=cost(2 * hidden.size * width, 2 * units * width),
        compiler_params=pltpu.CompilerParams(vmem_limit_bytes=8 * 2**20),
        name="down_more",
    )(hidden, *some)


def place_kernel(form, blocks, *refs):
    (_,), some, (down_out, held, sem_in, sem_out) = split(refs, 1, len(form.sources(blocks)))
    waits = form.loads(blocks, some, held, sem_in)
    stores = form.stores(blocks, held, down_out, sem_out)
    for wait, store in zip(waits, stores):
        wait()
        store.start()
    for store in stores:
        store.wait()


def place(form, blocks, ready, tables):
    some = form.operands(blocks, tables)
    units = ready.shape[0]
    width = form.widths(blocks)
    return pl.pallas_call(
        functools.partial(place_kernel, form, blocks),
        out_shape=jax.ShapeDtypeStruct(ready.shape, ready.dtype),
        in_specs=[ANY] * (len(some) + 1),
        out_specs=ANY,
        scratch_shapes=[
            pltpu.VMEM((units, width), BF16),
            pltpu.SemaphoreType.DMA((len(blocks),)),
            pltpu.SemaphoreType.DMA((len(blocks),)),
        ],
        input_output_aliases={0: 0},
        cost_estimate=cost(0, 4 * units * width),
        compiler_params=pltpu.CompilerParams(vmem_limit_bytes=8 * 2**20),
        name="place",
    )(ready, *some)


def mixed_blocks(form, blocks, tokens_ref, bufs):
    out = []
    for block, start, width in form.spans(blocks):
        cols = at(form.column(block), width)
        total = sum(buf[:, start:start + width].astype(F32) for buf in bufs)
        wide = tokens_ref[:, cols].astype(F32)
        out.append((cols, jnp.sqrt(F32(2.0)) * wide + 0.5 * total))
    return out


def mix_kernel(form, parts, n_tok, *refs):
    tokens_ref, *bufs, out_ref = refs
    n = 0
    for p, blocks in enumerate(parts):
        some = bufs[p * n_tok:(p + 1) * n_tok]
        for _, value in mixed_blocks(form, blocks, tokens_ref, some):
            out_ref[:, n:n + value.shape[1]] = value
            n += value.shape[1]


def mix(form, parts, tokens, values):
    flat = [x for some in values for x in some]
    width = sum(form.widths(blocks) for blocks in parts)
    return pl.pallas_call(
        functools.partial(mix_kernel, form, parts, len(values[0])),
        out_shape=jax.ShapeDtypeStruct((tokens.shape[0], width), F32),
        in_specs=[VMEM] * (1 + len(flat)),
        out_specs=VMEM,
        cost_estimate=cost(8 * tokens.shape[0] * width, 12 * tokens.shape[0] * width),
        compiler_params=pltpu.CompilerParams(vmem_limit_bytes=8 * 2**20),
        name="mix",
    )(tokens, *flat)


def finish_kernel(form, soon, late, *refs):
    tokens_ref, gain_ref, bias_ref, head_ref, *bufs, out_ref = refs
    width = tokens_ref.shape[-1]
    mixed = [
        (at(form.column(block), size), head_ref[:, start:start + size])
        for block, start, size in form.spans(soon)
    ]
    mixed += mixed_blocks(form, late, tokens_ref, bufs)
    center = sum(jnp.sum(m, axis=-1, keepdims=True) for _, m in mixed) / width
    spread = sum(jnp.sum(jnp.square(m - center), axis=-1, keepdims=True) for _, m in mixed) / width
    scale = lax.rsqrt(spread + 1e-05)
    for cols, m in mixed:
        out_ref[:, cols] = ((m - center) * scale * gain_ref[:, cols] + bias_ref[:, cols]).astype(BF16)


def finish_all(form, soon, late, tokens, gain, bias, head, parts):
    return pl.pallas_call(
        functools.partial(finish_kernel, form, soon, late),
        out_shape=jax.ShapeDtypeStruct(tokens.shape, BF16),
        in_specs=[VMEM] * (4 + len(parts)),
        out_specs=VMEM,
        cost_estimate=cost(16 * tokens.size, 16 * tokens.size),
        compiler_params=pltpu.CompilerParams(vmem_limit_bytes=8 * 2**20),
        name="finish",
    )(tokens, gain, bias, head, *parts)


def over_tp(blocks, n_tok):
    return [blocks[0]] + [
        lax.ppermute(blocks[d], "tp", [(i, i ^ d) for i in range(n_tok)])
        for d in range(1, n_tok)
    ]


def exchanged(sizes, tokens, gate_master, up_master, down_master, norm_gain, post_gain, post_bias):
    groups, n_tok = sizes["grp"], sizes["tp"]
    line = Line(sizes["fs"])
    gate, up, down = gate_master.T, up_master.T, down_master.T
    gain = norm_gain[None, :]
    last = line.count - 2
    most = tuple(range(last))

    whole = down.shape[1]
    half, cut = whole // groups, whole // groups // 2
    mine, other = 0, 1

    tables = {}
    for tag, width, cuts, *operands in (
        ("d", cut, ((mine, 0),), down),
        ("g", half, ((mine, 0),), gate, gain),
        ("u", half, ((mine, 0),), up, gain),
        ("e", cut, ((mine, 1), (other, 1)), down),
    ):
        halves = half_pieces(groups, width, cuts, *operands)
        tables[tag] = line_exchange(line, halves, sizes)
    pair_tables = (*tables["g"], *tables["u"])
    toks = over_tp([norm(tokens)] * n_tok, n_tok)
    gate_ready, up_ready, so_far = pair_part(line, most, toks, pair_tables, [gate, up, gain], None)
    gate_ready, up_ready, hidden = pair_part(
        line, (last,), toks, pair_tables, None,
        [so_far, gate_ready, up_ready],
    )
    form = Blocks(line, groups, whole, cut)
    down_tables = (tables["d"], tables["e"])
    early = ((OWN,), (0, mine, 0), (0, other, 0), *((k, mine, 0) for k in most[1:]), (0, mine, 1))
    late = ((0, other, 1), (last, other, 1))
    between = tuple(
        block
        for block in ((k, s, n) for n in (0, 1) for k in range(last + 1) for s in (mine, other))
        if block not in early and block not in late
    )
    down_ready, *own = down_own(form, early, n_tok, hidden, down_tables, down)
    own = over_tp(own, n_tok)
    rest = down_more(form, between, n_tok, hidden, down_tables)
    rest = over_tp(rest, n_tok)
    end = down_more(form, late, n_tok, hidden, down_tables)
    end = over_tp(end, n_tok)
    down_ready = place(form, between + late, down_ready, down_tables)
    head = mix(form, (early, between), tokens, (own, rest))
    result = finish_all(
        form, early + between, late, tokens,
        post_gain[None, :], post_bias[None, :], head, end,
    )
    return (gate_ready.T, up_ready.T, down_ready.T, result)


def fits(sizes, tokens, gate_master):
    groups, n_fs, n_tok = sizes["grp"], sizes["fs"], sizes["tp"]
    rows = gate_master.shape[0] // n_fs
    units = gate_master.shape[1] // n_tok
    return (
        groups == 2
        and 2 < n_fs <= LONGEST_LINE
        and n_tok > 1
        and n_tok & (n_tok - 1) == 0
        and rows % (groups * 2 * LANES) == 0
        and units % 16 == 0
        and tokens.shape[0] // (groups * n_fs * n_tok) % 16 == 0
    )


def solution(mesh):
    sizes = dict(mesh.shape)
    rows = P(("grp", "fs", "tp"), None)
    ready = P("grp", "tp")

    def over_mesh(body):
        return jax.shard_map(
            body,
            mesh=mesh,
            in_specs=(rows, P("fs", "tp"), P("fs", "tp"), P("fs", "tp"), P(), P(), P()),
            out_specs=(ready, ready, ready, rows),
            check_vma=False,
        )

    def run(tokens, gate_master, *rest):
        if not fits(sizes, tokens, gate_master):
            return over_mesh(plain)(tokens, gate_master, *rest)
        step = over_mesh(functools.partial(exchanged, sizes))
        return step(tokens, gate_master, *rest)

    return run
```

```python
import functools

import jax
import jax.numpy as jnp
from jax import lax
from jax.experimental import pallas as pl
from jax.experimental.pallas import tpu as pltpu
from jax.sharding import PartitionSpec as P


BF16 = jnp.bfloat16
F32 = jnp.float32
ANY = pl.BlockSpec(memory_space=pl.ANY)
HBM = pl.BlockSpec(memory_space=pltpu.HBM)
VMEM = pl.BlockSpec(memory_space=pltpu.VMEM)
LANES = 128
LONGEST_LINE = 8


def finish(wide, branch, post_gain, post_bias):
    mixed = jnp.sqrt(jnp.float32(2.0)) * wide + 0.5 * branch
    center = jnp.mean(mixed, axis=-1, keepdims=True)
    spread = jnp.mean(jnp.square(mixed - center), axis=-1, keepdims=True)
    return ((mixed - center) * lax.rsqrt(spread + 1e-05) * post_gain + post_bias).astype(
        jnp.bfloat16
    )


def plain(tokens, gate_master, up_master, down_master, norm_gain, post_gain, post_bias):
    row_count = gate_master.shape[0]
    first_row = lax.axis_index("fs") * row_count
    gain_rows = lax.dynamic_slice_in_dim(norm_gain, first_row, row_count, 0)
    gate_piece = (gain_rows[:, None] * gate_master).astype(BF16)
    up_piece = (gain_rows[:, None] * up_master).astype(BF16)
    down_piece = down_master.astype(BF16)
    gate_ready, up_ready, down_ready = (
        lax.all_gather(gate_piece, "fs", axis=0, tiled=True),
        lax.all_gather(up_piece, "fs", axis=0, tiled=True),
        lax.all_gather(down_piece, "fs", axis=0, tiled=True),
    )
    wide = tokens.astype(F32)
    normed = (wide * lax.rsqrt(jnp.mean(wide * wide, axis=-1, keepdims=True) + 1e-06)).astype(BF16)
    piece = lax.all_gather(normed, "tp", axis=0, tiled=True)
    gate = jnp.dot(piece, gate_ready, preferred_element_type=F32)
    upward = jnp.dot(piece, up_ready, preferred_element_type=F32)
    hidden = (jax.nn.silu(gate) * upward).astype(BF16)
    branch = lax.psum_scatter(
        lax.dot_general(
            hidden, down_ready, (((1,), (1,)), ((), ())), preferred_element_type=F32
        ).astype(BF16),
        "tp",
        scatter_dimension=0,
        tiled=True,
    ).astype(F32)
    return (gate_ready, up_ready, down_ready, finish(wide, branch, post_gain, post_bias))


class Line:
    def __init__(self, count):
        self.count = count
        self.swaps = []
        self.pairs = {}
        self.brings = {}
        for t in range(1, count):
            for q in (0, 1):
                pairs, brings = [], {}
                for i in range(q, count - 1, 2):
                    if i - t + 1 >= 0:
                        pairs.append((i, i + 1))
                        brings[i + 1] = i + 1 - t
                    if i + t < count:
                        pairs.append((i + 1, i))
                        brings[i] = i + t
                if pairs:
                    self.swaps.append((t, q))
                    self.pairs[t, q] = pairs
                    self.brings[t, q] = brings
        self.order = {f: [s for s in self.swaps if f in self.brings[s]] for f in range(count)}
        self.slots = [
            sorted({self.order[f][k] for f in range(count)}) for k in range(count - 1)
        ]

    def piece(self, f, k):
        out = jnp.int32(0)
        for i in range(self.count):
            s = self.order[i][k]
            out = jnp.where(f == i, jnp.int32(self.brings[s][i]), out)
        return out

    def holds(self, f, k, s):
        out = f < 0
        for i in range(self.count):
            if self.order[i][k] == s:
                out = jnp.logical_or(out, f == i)
        return out


MESH = ("grp", "fs", "tp")


def whole_moves(sizes, step):
    groups, n_fs, n_tok = (sizes[axis] for axis in MESH)

    def index(g, f, t):
        return (g * n_fs + f) * n_tok + t

    moves = []
    for g in range(groups):
        for f in range(n_fs):
            to = step(g, f)
            for t in range(n_tok):
                target = index(g, f, t ^ 1) if to is None else index(*to, t)
                moves.append((index(g, f, t), target))
    return moves


def line_exchange(line, halves, sizes):
    near, far = {}, {}
    for t, q in line.swaps:
        ends = {i for pair in line.pairs[t, q] for i in pair}

        def along(g, f):
            return (g, f + 1 if f % 2 == q else f - 1) if f in ends else None

        def across(g, f):
            return ((g + 1) % sizes["grp"], f) if f in line.brings[t, q] else None

        operand = halves[0] if t == 1 else near[t - 1, 1 - q]
        near[t, q] = lax.ppermute(operand, MESH, whole_moves(sizes, along))
        if t == 1 and len(halves) > 1:
            far[t, q] = lax.ppermute(halves[1], MESH, whole_moves(sizes, along))
        else:
            far[t, q] = lax.ppermute(near[t, q], MESH, whole_moves(sizes, across))
    return near, far


def at(start, size):
    return pl.ds(pl.multiple_of(start, LANES), size)


def cost(flops, moved):
    return pl.CostEstimate(flops=flops, bytes_accessed=moved, transcendentals=0)


def half_kernel(groups, cuts, *refs):
    *operands, buf, sem = refs
    master_ref, outs = operands[0], operands[-len(cuts):]
    whole = master_ref.shape[-1]
    width = outs[0].shape[-1]
    g, f = lax.axis_index("grp"), lax.axis_index("fs")
    starts = [(1 - g if side else g) * (whole // groups) + n * width for side, n in cuts]
    loads = [
        pltpu.make_async_copy(master_ref.at[:, at(start, width)], buf.at[n], sem.at[n])
        for n, start in enumerate(starts)
    ]
    for load in loads:
        load.start()
    for n, load in enumerate(loads):
        load.wait()
        value = buf[n]
        if len(operands) > len(cuts) + 1:
            value = value * operands[1][:, at(f * whole + starts[n], width)]
        outs[n][...] = value.astype(BF16)


def half_pieces(groups, width, cuts, master, gain=None):
    units = master.shape[0]
    count = len(cuts)
    operands = [master] if gain is None else [master, gain]
    return pl.pallas_call(
        functools.partial(half_kernel, groups, cuts),
        out_shape=(jax.ShapeDtypeStruct((units, width), BF16),) * count,
        in_specs=[HBM if gain is None and count == 1 else ANY, VMEM][: len(operands)],
        out_specs=(VMEM,) * count,
        scratch_shapes=[
            pltpu.VMEM((count, units, width), F32),
            pltpu.SemaphoreType.DMA((count,)),
        ],
        cost_estimate=cost(2**32, 6 * units * width * count),
        compiler_params=pltpu.CompilerParams(vmem_limit_bytes=8 * 2**20),
        name="half_pieces",
    )(*operands)


def norm_kernel(tokens_ref, out_ref):
    wide = tokens_ref[...].astype(F32)
    scale = lax.rsqrt(jnp.mean(wide * wide, axis=-1, keepdims=True) + 1e-06)
    out_ref[...] = (wide * scale).astype(BF16)


def norm(tokens):
    return pl.pallas_call(
        norm_kernel,
        out_shape=jax.ShapeDtypeStruct(tokens.shape, BF16),
        in_specs=[VMEM],
        out_specs=VMEM,
        cost_estimate=cost(4 * tokens.size, 4 * tokens.size),
        compiler_params=pltpu.CompilerParams(vmem_limit_bytes=8 * 2**20),
        name="norm_tokens",
    )(tokens)


def slot_loads(line, f, k, refs, fill, sem):
    swaps = line.slots[k]

    def each(act):
        for s in swaps:
            if len(swaps) == 1:
                act(pltpu.make_async_copy(refs[s], fill, sem))
            else:

                @pl.when(line.holds(f, k, s))
                def _():
                    act(pltpu.make_async_copy(refs[s], fill, sem))

    return (lambda: each(lambda c: c.start())), (lambda: each(lambda c: c.wait()))


def taken(line, ks):
    return sorted({s for k in ks for s in line.slots[k]})


def split(refs, *counts):
    out = []
    for n in counts:
        out.append(refs[:n])
        refs = refs[n:]
    return (*out, refs)


def pair_kernel(line, ks, own, n_tok, *refs):
    swaps = taken(line, ks)
    toks, refs = split(refs, n_tok)
    tables = []
    for _ in range(4):
        some, refs = split(refs, len(swaps))
        tables.append(dict(zip(swaps, some)))
    if own:
        (gate_ref, up_ref, gain_ref), refs = split(refs, 3)
    else:
        (so_far, _, _), refs = split(refs, 3)
    gate_out, up_out, out_ref, normed, held, masters, sem_in, sem_m, sem_t, sem_out = refs
    g, f = lax.axis_index("grp"), lax.axis_index("fs")
    whole = toks[0].shape[-1] // line.count
    half = tables[0][swaps[0]].shape[-1]
    rows = toks[0].shape[0]
    first = 1 if own else 0
    places = ([f] if own else []) + [line.piece(f, k) for k in ks]
    mine = []
    if own:
        mine = [
            pltpu.make_async_copy(src, masters.at[n], sem_m.at[n])
            for n, src in enumerate((gate_ref, up_ref))
        ]
    for load in mine:
        load.start()
    loads = []
    for i, k in enumerate(ks):
        for n, table in enumerate(tables):
            h = 1 - g if n % 2 else g
            fill = held.at[n // 2, :, at((first + i) * whole + h * half, half)]
            loads.append(slot_loads(line, f, k, table, fill, sem_in.at[4 * i + n]))
    token_loads = [
        pltpu.make_async_copy(
            tok.at[:, at(place * whole, whole)],
            normed.at[pl.ds(d * rows, rows), pl.ds(i * whole, whole)],
            sem_t.at[d * len(places) + i],
        )
        for d, tok in enumerate(toks)
        for i, place in enumerate(places)
    ]
    for load in token_loads:
        load.start()
    for begin, _ in loads:
        begin()
    stores = [
        [
            pltpu.make_async_copy(
                held.at[n, :, pl.ds(i * whole, whole)],
                out.at[:, at(place * whole, whole)],
                sem_out.at[2 * i + n],
            )
            for n, out in enumerate((gate_out, up_out))
        ]
        for i, place in enumerate(places)
    ]
    if own:
        gain = gain_ref[:, at(f * whole, whole)]
        for n, load in enumerate(mine):
            load.wait()
            held[n, :, :whole] = (masters[n] * gain).astype(BF16)
            stores[0][n].start()
    for i in range(len(ks)):
        for _, end in loads[4 * i:4 * i + 4]:
            end()
        for store in stores[first + i]:
            store.start()
    for load in token_loads:
        load.wait()
    gate, up = [
        lax.dot_general(
            normed[...], held[n], (((1,), (1,)), ((), ())), preferred_element_type=F32
        )
        for n in range(2)
    ]
    if own:
        out_ref[0] = gate
        out_ref[1] = up
    else:
        gate = gate + so_far[0]
        up = up + so_far[1]
        out_ref[...] = (gate / (1.0 + jnp.exp(-gate)) * up).astype(BF16)
    for some in stores:
        for store in some:
            store.wait()


def pair_part(line, ks, toks, tables, masters, so_far):
    own = so_far is None
    rows, width = toks[0].shape
    whole = width // line.count
    n_tok = len(toks)
    swaps = taken(line, ks)
    units = tables[0][swaps[0]].shape[0]
    blocks = len(ks) + (1 if own else 0)
    operands = [*toks, *(table[s] for table in tables for s in swaps)]
    in_specs = [ANY] * len(operands)
    aliases = {}
    if own:
        operands += masters
        in_specs += [ANY, ANY, VMEM]
        last = jax.ShapeDtypeStruct((2, n_tok * rows, units), F32)
    else:
        aliases = {len(operands) + 1: 0, len(operands) + 2: 1}
        operands += so_far
        in_specs += [VMEM, ANY, ANY]
        last = jax.ShapeDtypeStruct((n_tok * rows, units), BF16)
    ready = jax.ShapeDtypeStruct((units, width), BF16)
    return pl.pallas_call(
        functools.partial(pair_kernel, line, ks, own, n_tok),
        out_shape=(ready, ready, last),
        in_specs=in_specs,
        out_specs=(ANY, ANY, VMEM),
        scratch_shapes=[
            pltpu.VMEM((n_tok * rows, blocks * whole), BF16),
            pltpu.VMEM((2, units, blocks * whole), BF16),
            pltpu.VMEM((2, units, whole), F32),
            pltpu.SemaphoreType.DMA((4 * len(ks),)),
            pltpu.SemaphoreType.DMA((2,)),
            pltpu.SemaphoreType.DMA((n_tok * blocks,)),
            pltpu.SemaphoreType.DMA((2 * blocks,)),
        ],
        input_output_aliases=aliases,
        cost_estimate=cost(4 * n_tok * rows * units * blocks * whole, 10 * units * blocks * whole),
        compiler_params=pltpu.CompilerParams(vmem_limit_bytes=24 * 2**20),
        name="pair_first" if own else "pair_last",
    )(*operands)


OWN = -1


class Blocks:
    def __init__(self, line, groups, whole, cut):
        self.line, self.groups, self.whole, self.cut = line, groups, whole, cut

    def width(self, block):
        return self.whole if block[0] == OWN else self.cut

    def widths(self, blocks):
        return sum(self.width(block) for block in blocks)

    def spans(self, blocks):
        n = 0
        for block in blocks:
            yield block, n, self.width(block)
            n += self.width(block)

    def column(self, block):
        g, f = lax.axis_index("grp"), lax.axis_index("fs")
        if block[0] == OWN:
            return f * self.whole
        k, side, n = block
        half = (1 - g if side else g) * (self.whole // self.groups)
        return self.line.piece(f, k) * self.whole + half + n * self.cut

    def sources(self, blocks):
        return sorted(
            {(b[1], b[2], s) for b in blocks if b[0] != OWN for s in self.line.slots[b[0]]}
        )

    def operands(self, blocks, tables):
        return [tables[n][side][s] for side, n, s in self.sources(blocks)]

    def loads(self, blocks, refs, held, sem):
        f = lax.axis_index("fs")
        named = dict(zip(self.sources(blocks), refs))
        waits = []
        for i, (block, start, width) in enumerate(self.spans(blocks)):
            if block[0] == OWN:
                continue
            k, side, n = block
            table = {s: named[side, n, s] for s in self.line.slots[k]}
            begin, end = slot_loads(
                self.line, f, k, table, held.at[:, pl.ds(start, width)], sem.at[i]
            )
            begin()
            waits.append(end)
        return waits

    def stores(self, blocks, held, out, sem):
        return [
            pltpu.make_async_copy(
                held.at[:, pl.ds(start, width)], out.at[:, at(self.column(block), width)], sem.at[i]
            )
            for i, (block, start, width) in enumerate(self.spans(blocks))
        ]


def multiply(hidden_ref, held, start, stop, parts):
    rows = parts[0].shape[0]
    part = jnp.dot(
        hidden_ref[...], held[:, start:stop], preferred_element_type=F32
    ).astype(BF16)
    for d, ref in enumerate(parts):
        ref[:, start:stop] = part[d * rows:(d + 1) * rows]


def place_own_kernel(form, master, down_out, own_ref, wide, sem):
    mine = pltpu.make_async_copy(master, wide, sem.at[0])
    mine.start()
    mine.wait()
    own_ref[...] = wide[...].astype(BF16)
    store = pltpu.make_async_copy(
        own_ref, down_out.at[:, at(form.column((OWN,)), form.whole)], sem.at[1]
    )
    store.start()
    store.wait()


def place_own(form, master):
    units = master.shape[0]
    return pl.pallas_call(
        functools.partial(place_own_kernel, form),
        out_shape=(
            jax.ShapeDtypeStruct((units, form.whole * form.line.count), BF16),
            jax.ShapeDtypeStruct((units, form.whole), BF16),
        ),
        in_specs=[ANY],
        out_specs=(ANY, VMEM),
        scratch_shapes=[pltpu.VMEM((units, form.whole), F32), pltpu.SemaphoreType.DMA((2,))],
        cost_estimate=cost(units * form.whole, 8 * units * form.whole),
        compiler_params=pltpu.CompilerParams(vmem_limit_bytes=8 * 2**20),
        name="place_own",
    )(master)


def down_part_kernel(form, blocks, n_tok, *refs):
    mine = [n for n, block in enumerate(blocks) if block[0] == OWN]
    (hidden_ref,), own, some, parts, (held, sem_in) = split(
        refs, 1, len(mine), len(form.sources(blocks)), n_tok
    )
    loads = []
    for n in mine:
        start = form.widths(blocks[:n])
        loads.append(
            pltpu.make_async_copy(own[0], held.at[:, pl.ds(start, form.whole)], sem_in.at[n])
        )
    for load in loads:
        load.start()
    waits = form.loads(blocks, some, held, sem_in)
    for load in loads:
        load.wait()
    for wait in waits:
        wait()
    multiply(hidden_ref, held, 0, form.widths(blocks), parts)


def down_part(form, blocks, n_tok, hidden, tables, own=()):
    some = [*own, *form.operands(blocks, tables)]
    units = hidden.shape[1]
    rows = hidden.shape[0] // n_tok
    width = form.widths(blocks)
    return pl.pallas_call(
        functools.partial(down_part_kernel, form, blocks, n_tok),
        out_shape=(jax.ShapeDtypeStruct((rows, width), BF16),) * n_tok,
        in_specs=[VMEM] + [ANY] * len(some),
        out_specs=(VMEM,) * n_tok,
        scratch_shapes=[
            pltpu.VMEM((units, width), BF16),
            pltpu.SemaphoreType.DMA((len(blocks),)),
        ],
        cost_estimate=cost(2 * hidden.size * width, 2 * units * width),
        compiler_params=pltpu.CompilerParams(vmem_limit_bytes=8 * 2**20),
        name="down_part",
    )(hidden, *some)


def place_kernel(form, blocks, *refs):
    (_,), some, (down_out, held, sem_in, sem_out) = split(refs, 1, len(form.sources(blocks)))
    waits = form.loads(blocks, some, held, sem_in)
    stores = form.stores(blocks, held, down_out, sem_out)
    for wait, store in zip(waits, stores):
        wait()
        store.start()
    for store in stores:
        store.wait()


def place(form, blocks, ready, tables):
    some = form.operands(blocks, tables)
    units = ready.shape[0]
    width = form.widths(blocks)
    return pl.pallas_call(
        functools.partial(place_kernel, form, blocks),
        out_shape=jax.ShapeDtypeStruct(ready.shape, ready.dtype),
        in_specs=[ANY] * (len(some) + 1),
        out_specs=ANY,
        scratch_shapes=[
            pltpu.VMEM((units, width), BF16),
            pltpu.SemaphoreType.DMA((len(blocks),)),
            pltpu.SemaphoreType.DMA((len(blocks),)),
        ],
        input_output_aliases={0: 0},
        cost_estimate=cost(0, 4 * units * width),
        compiler_params=pltpu.CompilerParams(vmem_limit_bytes=8 * 2**20),
        name="place",
    )(ready, *some)


def mixed_blocks(form, blocks, tokens_ref, bufs):
    out = []
    for block, start, width in form.spans(blocks):
        cols = at(form.column(block), width)
        total = sum(buf[:, start:start + width].astype(F32) for buf in bufs)
        wide = tokens_ref[:, cols].astype(F32)
        out.append((cols, jnp.sqrt(F32(2.0)) * wide + 0.5 * total))
    return out


def mix_kernel(form, parts, n_tok, *refs):
    tokens_ref, *bufs, out_ref = refs
    n = 0
    for p, blocks in enumerate(parts):
        some = bufs[p * n_tok:(p + 1) * n_tok]
        for _, value in mixed_blocks(form, blocks, tokens_ref, some):
            out_ref[:, n:n + value.shape[1]] = value
            n += value.shape[1]


def mix(form, parts, tokens, values):
    flat = [x for some in values for x in some]
    width = sum(form.widths(blocks) for blocks in parts)
    return pl.pallas_call(
        functools.partial(mix_kernel, form, parts, len(values[0])),
        out_shape=jax.ShapeDtypeStruct((tokens.shape[0], width), F32),
        in_specs=[VMEM] * (1 + len(flat)),
        out_specs=VMEM,
        cost_estimate=cost(8 * tokens.shape[0] * width, 12 * tokens.shape[0] * width),
        compiler_params=pltpu.CompilerParams(vmem_limit_bytes=8 * 2**20),
        name="mix",
    )(tokens, *flat)


def finish_kernel(form, soon, late, *refs):
    tokens_ref, gain_ref, bias_ref, head_ref, *bufs, out_ref = refs
    width = tokens_ref.shape[-1]
    mixed = [
        (at(form.column(block), size), head_ref[:, start:start + size])
        for block, start, size in form.spans(soon)
    ]
    mixed += mixed_blocks(form, late, tokens_ref, bufs)
    center = sum(jnp.sum(m, axis=-1, keepdims=True) for _, m in mixed) / width
    spread = sum(jnp.sum(jnp.square(m - center), axis=-1, keepdims=True) for _, m in mixed) / width
    scale = lax.rsqrt(spread + 1e-05)
    for cols, m in mixed:
        out_ref[:, cols] = ((m - center) * scale * gain_ref[:, cols] + bias_ref[:, cols]).astype(BF16)


def finish_all(form, soon, late, tokens, gain, bias, head, parts):
    return pl.pallas_call(
        functools.partial(finish_kernel, form, soon, late),
        out_shape=jax.ShapeDtypeStruct(tokens.shape, BF16),
        in_specs=[VMEM] * (4 + len(parts)),
        out_specs=VMEM,
        cost_estimate=cost(16 * tokens.size, 16 * tokens.size),
        compiler_params=pltpu.CompilerParams(vmem_limit_bytes=8 * 2**20),
        name="finish",
    )(tokens, gain, bias, head, *parts)


def over_tp(blocks, n_tok):
    return [blocks[0]] + [
        lax.ppermute(blocks[d], "tp", [(i, i ^ d) for i in range(n_tok)])
        for d in range(1, n_tok)
    ]


def exchanged(sizes, tokens, gate_master, up_master, down_master, norm_gain, post_gain, post_bias):
    groups, n_tok = sizes["grp"], sizes["tp"]
    line = Line(sizes["fs"])
    gate, up, down = gate_master.T, up_master.T, down_master.T
    gain = norm_gain[None, :]
    last = line.count - 2
    most = tuple(range(last))

    whole = down.shape[1]
    half, cut = whole // groups, whole // groups // 2
    mine, other = 0, 1

    tables = {}
    for tag, width, cuts, *operands in (
        ("d", cut, ((mine, 0),), down),
        ("g", half, ((mine, 0),), gate, gain),
        ("u", half, ((mine, 0),), up, gain),
        ("e", cut, ((mine, 1), (other, 1)), down),
    ):
        halves = half_pieces(groups, width, cuts, *operands)
        tables[tag] = line_exchange(line, halves, sizes)
    pair_tables = (*tables["g"], *tables["u"])
    toks = over_tp([norm(tokens)] * n_tok, n_tok)
    gate_ready, up_ready, so_far = pair_part(line, most, toks, pair_tables, [gate, up, gain], None)
    gate_ready, up_ready, hidden = pair_part(
        line, (last,), toks, pair_tables, None,
        [so_far, gate_ready, up_ready],
    )
    form = Blocks(line, groups, whole, cut)
    down_tables = (tables["d"], tables["e"])
    early = ((OWN,), (0, mine, 0), (0, other, 0), *((k, mine, 0) for k in most[1:]), (0, mine, 1))
    late = ((0, other, 1), (last, other, 1))
    between = tuple(
        block
        for block in ((k, s, n) for n in (0, 1) for k in range(last + 1) for s in (mine, other))
        if block not in early and block not in late
    )
    down_ready, piece = place_own(form, down)
    own = down_part(form, early, n_tok, hidden, down_tables, [piece])
    own = over_tp(own, n_tok)
    rest = down_part(form, between, n_tok, hidden, down_tables)
    rest = over_tp(rest, n_tok)
    end = down_part(form, late, n_tok, hidden, down_tables)
    end = over_tp(end, n_tok)
    down_ready = place(form, early[1:] + between + late, down_ready, down_tables)
    head = mix(form, (early, between), tokens, (own, rest))
    result = finish_all(
        form, early + between, late, tokens,
        post_gain[None, :], post_bias[None, :], head, end,
    )
    return (gate_ready.T, up_ready.T, down_ready.T, result)


def fits(sizes, tokens, gate_master):
    groups, n_fs, n_tok = sizes["grp"], sizes["fs"], sizes["tp"]
    rows = gate_master.shape[0] // n_fs
    units = gate_master.shape[1] // n_tok
    return (
        groups == 2
        and 2 < n_fs <= LONGEST_LINE
        and n_tok > 1
        and n_tok & (n_tok - 1) == 0
        and rows % (groups * 2 * LANES) == 0
        and units % 16 == 0
        and tokens.shape[0] // (groups * n_fs * n_tok) % 16 == 0
    )


def solution(mesh):
    sizes = dict(mesh.shape)
    rows = P(("grp", "fs", "tp"), None)
    ready = P("grp", "tp")

    def over_mesh(body):
        return jax.shard_map(
            body,
            mesh=mesh,
            in_specs=(rows, P("fs", "tp"), P("fs", "tp"), P("fs", "tp"), P(), P(), P()),
            out_specs=(ready, ready, ready, rows),
            check_vma=False,
        )

    def run(tokens, gate_master, *rest):
        if not fits(sizes, tokens, gate_master):
            return over_mesh(plain)(tokens, gate_master, *rest)
        step = over_mesh(functools.partial(exchanged, sizes))
        return step(tokens, gate_master, *rest)

    return run
```
